32 devices in a mesh: ep: 8 (over z, core), tp: 4 (over y, x).
Axes of the slice: x: 2, y: 2, z: 4, core: 2. Of those that a mesh axis runs over, the one named last changes fastest.
Arguments:
- tokens: bfloat16 [384, 2048], P('ep'), may hold values from -6 to 6
- retention_state: float32 [384, 16, 64, 64], P('ep', 'tp'), may hold values from -1.5 to 1.5
- lengths: int32 [384], P('ep'), may hold values from 1024 to 16383
- query_weight: bfloat16 [2048, 1024], P(None, 'tp'), may hold values from -0.125 to 0.125
- key_weight: bfloat16 [2048, 1024], P(None, 'tp'), may hold values from -0.125 to 0.125
- value_weight: bfloat16 [2048, 1024], P(None, 'tp'), may hold values from -0.125 to 0.125
- gate_weight: bfloat16 [2048, 1024], P(None, 'tp'), may hold values from -0.125 to 0.125
- out_weight: bfloat16 [1024, 2048], P(None, 'tp'), may hold values from -0.1875 to 0.1875
- first_gain: float32 [2048], replicated, may hold values from 0.1 to 1.9
- routing: int32 [384, 4], P('ep'), may hold values from 0 to 31, all different within a row; in each aligned block of 48 rows (0 to 47, 48 to 95, ...) at most 18 rows name the same one
- route_weight: float32 [384, 4], P('ep'), may hold values from 0.1 to 1
- expert_gate: bfloat16 [32, 2048, 512], P('ep', None, 'tp'), may hold values from -0.125 to 0.125
- expert_up: bfloat16 [32, 2048, 512], P('ep', None, 'tp'), may hold values from -0.125 to 0.125
- expert_down: bfloat16 [32, 512, 2048], P('ep', None, 'tp'), may hold values from -0.25 to 0.25
- shared_gate: bfloat16 [2048, 512], P(None, 'tp'), may hold values from -0.125 to 0.125
- shared_up: bfloat16 [2048, 512], P(None, 'tp'), may hold values from -0.125 to 0.125
- shared_down: bfloat16 [512, 2048], P(None, 'tp'), may hold values from -0.25 to 0.25
- side_gate: bfloat16 [2048, 256], P('ep', 'tp'), may hold values from -0.125 to 0.125
- side_up: bfloat16 [2048, 256], P('ep', 'tp'), may hold values from -0.125 to 0.125
- side_down: bfloat16 [256, 2048], P(None, 'tp'), may hold values from -0.375 to 0.375
- side_switch: bfloat16 [2048], replicated, may hold values from -0.125 to 0.125
- second_gain: float32 [2048], P('tp'), may hold values from 0.1 to 1.9
Outputs:
- output: bfloat16 [384, 2048], P('ep', 'tp')
- new_state: float32 [384, 16, 64, 64], P('ep', 'tp')
The draws below stay inside these ranges and needn't reach their ends.
Inputs may be any that keep to these rules, and one draw needn't show every extreme that they name: `routing`: each row names 4 different experts. Among the rows of one ep index (aligned blocks of 48 rows) no expert is named by more than 18 rows, a bound that some block reaches.
All inputs are finite; a program needn't handle non-finite values.
Results may differ from the reference program's by a relative error of at most 0.013.
Values may be sent and summed in bfloat16 or wider, within the bound.
A program may use at most 64 MiB of HBM per device.

```python
import math
import jax
import jax.numpy as jnp
import numpy as np
from jax import lax

D = 2048
HEADS = 16
HEAD_SIZE = 64
FE = 512
SHARED_F = 512
DENSE_F = 256
TOPK = 4
SEQ_DEV = 48
BATCH = 384
EXPERTS = 32
CAP = 18
N_EP = 8


def touch_ends(array, own_key, low, largest):
    longest = array.shape.index(max(array.shape))
    spots = []
    for shift in (0, 1):
        where = [jax.random.randint(jax.random.fold_in(own_key, axis), (), 0, length) for axis, length in enumerate(array.shape)]
        where[longest] = (where[longest] + shift) % array.shape[longest]
        spots.append(tuple(where))
    return array.at[spots[0]].set(low).at[spots[1]].set(largest)


def levels(rng, extent, cuts, low, largest):
    level, own = 1.0, jax.random.fold_in(rng, 6)
    for dim, shards_of in cuts:
        steps = jnp.exp(jax.random.uniform(jax.random.fold_in(own, dim), (shards_of,), jnp.float32, low / len(cuts), largest / len(cuts)))
        level = level * jnp.repeat(steps, extent[dim] // shards_of).reshape([-1 if axis == dim else 1 for axis in range(len(extent))])
    return level


def assign_block(key, own, number, rows, number_of, top, bound, slope):
    ranking = jax.random.permutation(key, number_of)
    crowded, ordinary = portions_of(number_of, rows * top, bound, slope, True), portions_of(number_of, rows * top, bound, slope, False)
    places = jnp.arange(number_of)

    def named(sizes, offset_by):
        used = int((sizes > 0).sum())
        fixed = max(1, used // 4)
        shifted = fixed + (places - fixed + offset_by * (used - fixed)) % max(1, number_of - fixed)
        return jnp.zeros((number_of,), jnp.int32).at[ranking[jnp.where(places < fixed, places, shifted)]].set(jnp.asarray(sizes, jnp.int32))

    sizes = jnp.where(number % 4 == 0, named(crowded, number // 4), named(ordinary, number - number // 4 - 1))
    mixed = jax.random.permutation(jax.random.fold_in(own, 3), number_of)
    giver, receiver = mixed[0:number_of // 2 * 2:2], mixed[1:number_of // 2 * 2:2]
    room = jnp.minimum(sizes[giver] - 1, bound - sizes[receiver]) // 2
    room = jnp.where((giver == ranking[0]) | (receiver == ranking[0]) | (sizes[receiver] == 0), 0, jnp.maximum(room, 0))
    shifted = jax.random.randint(jax.random.fold_in(own, 4), (number_of // 2,), 0, 1 << 20) % (room + 1)
    sizes = sizes.at[giver].add(-shifted).at[receiver].add(shifted)
    items = jnp.searchsorted(jnp.cumsum(sizes), jnp.arange(rows * top), side="right").astype(jnp.int32)
    listing = items.reshape(top, rows).T
    listing = listing[jax.random.permutation(jax.random.fold_in(own, 1), rows)]
    offset_by = jax.random.randint(jax.random.fold_in(own, 2), (rows, 1), 0, top)
    return jnp.take_along_axis(listing, (jnp.arange(top)[None, :] + offset_by) % top, axis=1)


def portions_of(count, total, most, lean, full):
    weights = [(1 << 20) // math.isqrt(standing ** lean) + 1 for standing in range(1, count + 1)]
    largest = most if full else min(most, max(-(-total // count), total * weights[0] // sum(weights)))
    least = 1 if total - largest >= count - 1 else 0
    given, rest = [largest] + [least] * (count - 1), total - largest - least * (count - 1)
    while rest > 0:
        movable = [i for i in range(1, count) if given[i] < largest] or [i for i in range(1, count) if given[i] < most]
        whole, left = sum([weights[i] for i in movable]), rest
        for i in movable:
            addition = min(most - given[i], max(1, left * weights[i] // whole), rest)
            given[i] = given[i] + addition
            rest = rest - addition
    return np.array(given)


def bell_draw(stream_key, shape, deviation, bound, shards=(), kind=jnp.bfloat16):
    array = jax.random.normal(stream_key, shape, jnp.float32) * deviation
    if len(shards) > 0:
        array = levels(stream_key, shape, shards, -0.22, 0.18) * array
    return jnp.clip(array, min=-bound, max=bound).astype(kind)


def setup_inputs(seed: int = 0) -> dict:
    key_list = jax.random.split(jax.random.key(seed), 23)
    tokens = bell_draw(key_list[0], (BATCH, D), 1.0, 6.0, ((0, 8),))
    retention_state = bell_draw(key_list[1], (BATCH, HEADS, HEAD_SIZE, HEAD_SIZE), 0.25, 1.5, ((0, 8), (1, 4)), jnp.float32)
    lengths = touch_ends(jax.random.randint(key_list[2], (BATCH,), 1024, 16384), jax.random.fold_in(key_list[2], 1), 1024, 16383).astype(jnp.int32)
    query_weight = bell_draw(key_list[3], (D, HEADS * HEAD_SIZE), D ** -0.5, 0.125, ((1, 4),))
    key_weight = bell_draw(key_list[4], (D, HEADS * HEAD_SIZE), D ** -0.5, 0.125, ((1, 4),))
    value_weight = bell_draw(key_list[5], (D, HEADS * HEAD_SIZE), D ** -0.5, 0.125, ((1, 4),))
    gate_weight = bell_draw(key_list[6], (D, HEADS * HEAD_SIZE), D ** -0.5, 0.125, ((1, 4),))
    out_weight = bell_draw(key_list[7], (HEADS * HEAD_SIZE, D), (HEADS * HEAD_SIZE) ** -0.5, 0.1875, ((1, 4),))
    first_gain = jnp.clip(1.0 + 0.18 * jax.random.normal(key_list[8], (D,), jnp.float32), 0.1, 1.9)
    routing_keys = jax.random.split(jax.random.fold_in(key_list[9], 1), BATCH // SEQ_DEV)
    routing_turns = jax.random.permutation(jax.random.fold_in(key_list[9], 3), BATCH // SEQ_DEV)
    routing = jax.vmap(lambda own, number: assign_block(jax.random.fold_in(key_list[9], 2), own, number, SEQ_DEV, EXPERTS, TOPK, CAP, 2))(routing_keys, routing_turns).reshape((BATCH, TOPK))
    route_weight = jnp.clip(0.1 + 0.9 * jax.random.uniform(key_list[10], (BATCH, TOPK), jnp.float32) ** levels(key_list[10], (BATCH, TOPK), ((0, 8),), -0.2, 0.2), 0.1, 1.0)
    expert_gate = bell_draw(key_list[11], (EXPERTS, D, FE), D ** -0.5, 0.125, ((0, 8), (2, 4)))
    expert_up = bell_draw(key_list[12], (EXPERTS, D, FE), D ** -0.5, 0.125, ((0, 8), (2, 4)))
    expert_down = bell_draw(key_list[13], (EXPERTS, FE, D), FE ** -0.5, 0.25, ((0, 8), (2, 4)))
    shared_gate = bell_draw(key_list[14], (D, SHARED_F), D ** -0.5, 0.125, ((1, 4),))
    shared_up = bell_draw(key_list[15], (D, SHARED_F), D ** -0.5, 0.125, ((1, 4),))
    shared_down = bell_draw(key_list[16], (SHARED_F, D), SHARED_F ** -0.5, 0.25, ((1, 4),))
    side_gate = bell_draw(key_list[17], (D, DENSE_F), D ** -0.5, 0.125, ((0, 8), (1, 4)))
    side_up = bell_draw(key_list[18], (D, DENSE_F), D ** -0.5, 0.125, ((0, 8), (1, 4)))
    side_down = bell_draw(key_list[19], (DENSE_F, D), DENSE_F ** -0.5, 0.375, ((1, 4),))
    side_switch = bell_draw(key_list[20], (D,), D ** -0.5, 0.125)
    second_gain = jnp.clip(1.0 + 0.18 * jax.random.normal(key_list[21], (D,), jnp.float32), 0.1, 1.9)
    return {"tokens": tokens, "retention_state": retention_state, "lengths": lengths, "query_weight": query_weight, "key_weight": key_weight, "value_weight": value_weight, "gate_weight": gate_weight, "out_weight": out_weight, "first_gain": first_gain, "routing": routing, "route_weight": route_weight, "expert_gate": expert_gate, "expert_up": expert_up, "expert_down": expert_down, "shared_gate": shared_gate, "shared_up": shared_up, "shared_down": shared_down, "side_gate": side_gate, "side_up": side_up, "side_down": side_down, "side_switch": side_switch, "second_gain": second_gain}


RESIDUAL_SCALE = 2.0 ** 0.25
NORM_EPS = 1e-05
GROUP_EPS = 1e-06
ROPE_BASE = 10000.0

def rotate(vector, positions):
    half_width = vector.shape[-1] // 2
    frequency = ROPE_BASE ** (-jnp.arange(half_width, dtype=jnp.float32) / half_width)
    angles = positions.astype(jnp.float32)[:, None, None] * frequency[None, None, :]
    cosine = jnp.cos(angles)
    sine_part = jnp.sin(angles)
    first_half = vector[..., :half_width]
    second_half = vector[..., half_width:]
    return jnp.concatenate([first_half * cosine - second_half * sine_part, second_half * cosine + first_half * sine_part], -1)

def retain(tokens, retention_state, lengths, query_weight, key_weight, value_weight, gate_weight, first_head):
    row_count = tokens.shape[0]
    head_count = retention_state.shape[1]
    head_width = retention_state.shape[2]

    def project(weight):
        rounded = jnp.dot(tokens, weight, preferred_element_type=jnp.float32).astype(jnp.bfloat16)
        return lax.optimization_barrier(rounded).astype(jnp.float32)
    queries = rotate(project(query_weight).reshape(row_count, head_count, head_width), lengths)
    key_rows = rotate(project(key_weight).reshape(row_count, head_count, head_width), lengths) * head_width ** (-0.5)
    values = project(value_weight).reshape(row_count, head_count, head_width)
    gate_act = project(gate_weight)
    head_index = (first_head + jnp.arange(head_count)).astype(jnp.float32)
    decays = 1.0 - 2.0 ** (-5.0 - 7.0 * head_index / (HEADS - 1))
    own_term = lax.optimization_barrier(jnp.sum(queries * key_rows, -1, keepdims=True)) * values
    carried = decays[None, :, None] * jnp.einsum('bhd,bhde->bhe', queries, retention_state, precision=lax.Precision.HIGHEST)
    result = own_term + carried
    new_state = decays[None, :, None, None] * retention_state + key_rows[:, :, :, None] * values[:, :, None, :]
    normed = result * lax.rsqrt(lax.optimization_barrier(jnp.mean(result * result, -1, keepdims=True)) + GROUP_EPS)
    mixed_heads = (normed.reshape(row_count, head_count * head_width) * jax.nn.silu(gate_act)).astype(jnp.bfloat16)
    return (mixed_heads, new_state)

def layer_norm(values, gain):
    row_mean = lax.optimization_barrier(jnp.mean(values, -1, keepdims=True))
    square = lax.optimization_barrier(jnp.mean(values * values, -1, keepdims=True))
    return ((values - row_mean) * lax.rsqrt(square - row_mean * row_mean + NORM_EPS) * gain).astype(jnp.bfloat16)

def slot_numbers(route_ids, expert_count, capacity):
    onehot = (route_ids[..., None] == jnp.arange(expert_count, dtype=jnp.int32)).astype(jnp.int32)
    position = lax.optimization_barrier(jnp.sum(jnp.cumsum(onehot, -2) * onehot, -1)) - 1
    return route_ids * capacity + position

def take_rows(source_rows, row_index):
    return source_rows[row_index]

def one_expert(operands):
    rows_in, gate_mat, up_mat, down_mat = operands
    gate_part = jnp.dot(rows_in, gate_mat, preferred_element_type=jnp.float32)
    up_part = jnp.dot(rows_in, up_mat, preferred_element_type=jnp.float32)
    hidden = (jax.nn.silu(gate_part) * up_part).astype(jnp.bfloat16)
    return jnp.dot(hidden, down_mat, preferred_element_type=jnp.float32).astype(jnp.bfloat16)

def reference(tokens, retention_state, lengths, query_weight, key_weight, value_weight, gate_weight, out_weight, first_gain, routing, route_weight, expert_gate, expert_up, expert_down, shared_gate, shared_up, shared_down, side_gate, side_up, side_down, side_switch, second_gain):
    mixed_heads, new_state = retain(tokens, retention_state, lengths, query_weight, key_weight, value_weight, gate_weight, 0)
    mixing = jnp.dot(mixed_heads, out_weight, preferred_element_type=jnp.float32)
    normed = layer_norm(RESIDUAL_SCALE * tokens.astype(jnp.float32) + mixing, first_gain)
    shared_hidden = (jax.nn.silu(jnp.dot(normed, shared_gate, preferred_element_type=jnp.float32)) * jnp.dot(normed, shared_up, preferred_element_type=jnp.float32)).astype(jnp.bfloat16)
    shared_out = jnp.dot(shared_hidden, shared_down, preferred_element_type=jnp.float32)
    side_hidden = (jax.nn.silu(jnp.dot(normed, side_gate, preferred_element_type=jnp.float32)) * jnp.dot(normed, side_up, preferred_element_type=jnp.float32)).astype(jnp.bfloat16)
    side_out = jnp.dot(side_hidden, side_down, preferred_element_type=jnp.float32)
    switch = jax.nn.sigmoid(jnp.dot(normed, side_switch, preferred_element_type=jnp.float32))
    assigned = SEQ_DEV * TOPK
    groups = routing.reshape(N_EP, assigned)
    slot_ids = slot_numbers(groups, EXPERTS, CAP)
    owners = jnp.arange(assigned, dtype=jnp.int32) // TOPK
    table = jnp.full((N_EP, EXPERTS * CAP), SEQ_DEV, jnp.int32)
    table = table.at[jnp.arange(N_EP, dtype=jnp.int32)[:, None], slot_ids].set(jnp.broadcast_to(owners[None, :], (N_EP, assigned)))
    padded = jnp.concatenate([normed.reshape(N_EP, SEQ_DEV, D), jnp.zeros((N_EP, 1, D), jnp.bfloat16)], 1)
    slot_rows = jax.vmap(take_rows)(padded, table)
    per_expert = jnp.transpose(slot_rows.reshape(N_EP, EXPERTS, CAP, D), (1, 0, 2, 3)).reshape(EXPERTS, N_EP * CAP, D)
    outputs = lax.map(one_expert, (per_expert, expert_gate, expert_up, expert_down))
    back = jnp.transpose(outputs.reshape(EXPERTS, N_EP, CAP, D), (1, 0, 2, 3)).reshape(N_EP, EXPERTS * CAP, D)
    picked = jax.vmap(take_rows)(back, slot_ids).reshape(BATCH, TOPK, D)
    routed = lax.optimization_barrier(jnp.sum(picked.astype(jnp.float32) * route_weight[:, :, None], 1))
    pre_second = RESIDUAL_SCALE * normed.astype(jnp.float32) + routed + shared_out + switch[:, None] * side_out
    output = layer_norm(pre_second, second_gain)
    return (output, new_state)
```

```python
import functools

import jax
import jax.numpy as jnp
from jax import lax
from jax.experimental import pallas as pl
from jax.experimental.pallas import tpu as pltpu
from jax.sharding import PartitionSpec as P

HEADS = 16


RESIDUAL_SCALE = 2.0**0.25
NORM_EPS = 1e-05
GROUP_EPS = 1e-06
ROPE_BASE = 10000.0


def rotate(vector, positions):
    half_width = vector.shape[-1] // 2
    frequency = ROPE_BASE ** (-jnp.arange(half_width, dtype=jnp.float32) / half_width)
    angles = positions.astype(jnp.float32)[:, None, None] * frequency[None, None, :]
    cosine = jnp.cos(angles)
    sine_part = jnp.sin(angles)
    first_half = vector[..., :half_width]
    second_half = vector[..., half_width:]
    return jnp.concatenate(
        [
            first_half * cosine - second_half * sine_part,
            second_half * cosine + first_half * sine_part,
        ],
        -1,
    )


def retain(
    retention_state,
    lengths,
    projections,
    first_head,
):
    row_count = retention_state.shape[0]
    head_count = retention_state.shape[1]
    head_width = retention_state.shape[2]

    query_rows, key_part, value_part, gate_part = [part.astype(jnp.float32) for part in projections]
    queries = rotate(query_rows.reshape(row_count, head_count, head_width), lengths)
    key_rows = rotate(
        key_part.reshape(row_count, head_count, head_width), lengths
    ) * head_width ** (-0.5)
    values = value_part.reshape(row_count, head_count, head_width)
    gate_act = gate_part
    head_index = (first_head + jnp.arange(head_count)).astype(jnp.float32)
    decays = 1.0 - 2.0 ** (-5.0 - 7.0 * head_index / (HEADS - 1))
    own_term = jnp.sum(queries * key_rows, -1, keepdims=True) * values
    carried = decays[None, :, None] * jnp.sum(queries[:, :, :, None] * retention_state, 2)
    result = own_term + carried
    new_state = (
        decays[None, :, None, None] * retention_state
        + key_rows[:, :, :, None] * values[:, :, None, :]
    )
    normed = result * lax.rsqrt(jnp.mean(result * result, -1, keepdims=True) + GROUP_EPS)
    mixed_heads = (
        normed.reshape(row_count, head_count * head_width) * jax.nn.silu(gate_act)
    ).astype(jnp.bfloat16)
    return (mixed_heads, new_state)


VMEM = pl.BlockSpec(memory_space=pltpu.VMEM)
DEVICE = pl.DeviceIdType.MESH


def enter(peers):
    barrier = pltpu.get_barrier_semaphore()
    for peer in peers:
        pl.semaphore_signal(barrier, inc=1, device_id=peer, device_id_type=DEVICE)
    pl.semaphore_wait(barrier, len(peers))


def send(source, target, send_sem, recv_sem, peer):
    copy = pltpu.make_async_remote_copy(
        src_ref=source,
        dst_ref=target,
        send_sem=send_sem,
        recv_sem=recv_sem,
        device_id=peer,
        device_id_type=DEVICE,
    )
    copy.start()
    return copy


def on_axis(axis, index):
    if axis == "ep":
        return (index, lax.axis_index("tp"))
    return (lax.axis_index("ep"), index)


def gather_body(axis, count, parts, *refs):
    sources, targets = refs[:parts], refs[parts : 2 * parts]
    send_sem, recv_sem, local_sem = refs[2 * parts :]
    me = lax.axis_index(axis)
    others = [lax.rem(me + step, count) for step in range(1, count)]
    locals_ = []
    for part in range(parts):
        own = pltpu.make_async_copy(sources[part], targets[part].at[me], local_sem.at[part])
        own.start()
        locals_.append(own)
    enter([on_axis(axis, other) for other in others])
    copies = []
    for step, other in enumerate(others):
        for part in range(parts):
            copies.append(
                send(
                    sources[part],
                    targets[part].at[me],
                    send_sem.at[step, part],
                    recv_sem.at[step, part],
                    on_axis(axis, other),
                )
            )
    for copy in locals_:
        copy.wait()
    for copy in copies:
        copy.wait()


def gather(arrays, axis, ident):
    count, parts = lax.axis_size(axis), len(arrays)
    return pl.pallas_call(
        functools.partial(gather_body, axis, count, parts),
        out_shape=[jax.ShapeDtypeStruct((count,) + a.shape, a.dtype) for a in arrays],
        in_specs=[VMEM] * parts,
        out_specs=[VMEM] * parts,
        scratch_shapes=[
            pltpu.SemaphoreType.DMA((count - 1, parts)),
            pltpu.SemaphoreType.DMA((count - 1, parts)),
            pltpu.SemaphoreType.DMA((parts,)),
        ],
        compiler_params=pltpu.CompilerParams(collective_id=ident, has_side_effects=True),
    )(*arrays)


def scatter_body(count, source, target, send_sem, recv_sem, local_sem):
    me = lax.axis_index("ep")
    others = [lax.rem(me + step, count) for step in range(1, count)]
    own = pltpu.make_async_copy(source.at[me], target.at[me], local_sem)
    own.start()
    enter([on_axis("ep", other) for other in others])
    copies = [
        send(
            source.at[other],
            target.at[me],
            send_sem.at[step],
            recv_sem.at[step],
            on_axis("ep", other),
        )
        for step, other in enumerate(others)
    ]
    own.wait()
    for copy in copies:
        copy.wait()


def scatter(array, ident):
    count = array.shape[0]
    return pl.pallas_call(
        functools.partial(scatter_body, count),
        out_shape=jax.ShapeDtypeStruct(array.shape, array.dtype),
        in_specs=[VMEM],
        out_specs=VMEM,
        scratch_shapes=[
            pltpu.SemaphoreType.DMA((count - 1,)),
            pltpu.SemaphoreType.DMA((count - 1,)),
            pltpu.SemaphoreType.DMA,
        ],
        compiler_params=pltpu.CompilerParams(collective_id=ident, has_side_effects=True),
    )(array)


def first_body(count, *refs):
    parts = 3
    sources, (tokens, *weights) = refs[:parts], refs[parts : parts + 5]
    targets = refs[parts + 5 : 2 * parts + 5]
    results = refs[2 * parts + 5 : 2 * parts + 9]
    send_sem, recv_sem, local_sem = refs[2 * parts + 9 :]
    chips = count // 2
    me = lax.axis_index("ep")
    chip, core = me // 2, lax.rem(me, 2)
    partner = on_axis("ep", chip * 2 + 1 - core)
    line = [lax.rem(chip + step, chips) * 2 + core for step in range(1, chips)]
    senders = [lax.rem(chip + chips - step, chips) * 2 + core for step in range(1, chips)]
    locals_ = []
    for part in range(parts):
        own = pltpu.make_async_copy(sources[part], targets[part].at[me], local_sem.at[part])
        own.start()
        locals_.append(own)
    enter([on_axis("ep", other) for other in line] + [partner])
    direct, copies = [], []
    for step, other in enumerate(line):
        for part in range(parts):
            direct.append(
                send(
                    sources[part],
                    targets[part].at[me],
                    send_sem.at[step, part],
                    recv_sem.at[step, part],
                    on_axis("ep", other),
                )
            )
    for part in range(parts):
        copies.append(
            send(
                sources[part],
                targets[part].at[me],
                send_sem.at[chips - 1, part],
                recv_sem.at[chips - 1, part],
                partner,
            )
        )
    for weight, result in zip(weights, results):
        result[...] = jnp.dot(
            tokens[...], weight[...], preferred_element_type=jnp.float32
        ).astype(result.dtype)
    for step, sender in enumerate(senders):
        for part in range(parts):
            direct[step * parts + part].wait_recv()
            copies.append(
                send(
                    targets[part].at[sender],
                    targets[part].at[sender],
                    send_sem.at[chips + step, part],
                    recv_sem.at[chips + step, part],
                    partner,
                )
            )
    for copy in locals_:
        copy.wait()
    for copy in direct:
        copy.wait_send()
    for copy in copies:
        copy.wait()


def first(arrays, tokens, weights, ident):
    count, parts = lax.axis_size("ep"), len(arrays)
    rows = tokens.shape[0]
    return pl.pallas_call(
        functools.partial(first_body, count),
        out_shape=[jax.ShapeDtypeStruct((count,) + a.shape, a.dtype) for a in arrays]
        + [jax.ShapeDtypeStruct((rows, w.shape[1]), jnp.bfloat16) for w in weights],
        in_specs=[VMEM] * (parts + 5),
        out_specs=[VMEM] * (parts + 4),
        scratch_shapes=[
            pltpu.SemaphoreType.DMA((count - 1, parts)),
            pltpu.SemaphoreType.DMA((count - 1, parts)),
            pltpu.SemaphoreType.DMA((parts,)),
        ],
        compiler_params=pltpu.CompilerParams(collective_id=ident, has_side_effects=True),
    )(*arrays, tokens, *weights)


def spread_body(count, tp_count, source, target, send_sem, recv_sem, local_sem):
    chips, width = count // 2, source.shape[1]
    me, own_tp = lax.axis_index("ep"), lax.axis_index("tp")
    chip, core = me // 2, lax.rem(me, 2)
    partner = (chip * 2 + 1 - core, own_tp)

    def place(row, col):
        return target.at[row, :, pl.ds(pl.multiple_of(col * width, width), width)]

    def chip_at(step):
        return lax.rem(chip + chips + step, chips) * 2 + core

    def tp_at(step):
        return lax.rem(own_tp + tp_count + step, tp_count)

    own = pltpu.make_async_copy(source, place(me, own_tp), local_sem)
    own.start()
    line = [(chip_at(step), own_tp) for step in range(1, chips)]
    plane = [(me, tp_at(step)) for step in range(1, tp_count)]
    enter(line + plane + [partner])

    def pair(line_step, plane_step, to_partner):
        return (
            send_sem.at[to_partner, line_step, plane_step],
            recv_sem.at[to_partner, line_step, plane_step],
        )

    direct, planar, copies = [], {}, []
    for step in range(1, chips):
        direct.append(send(source, place(me, own_tp), *pair(step, 0, 0), line[step - 1]))
    for step in range(1, tp_count):
        planar[(0, step)] = send(source, place(me, own_tp), *pair(0, step, 0), plane[step - 1])
    copies.append(send(source, place(me, own_tp), *pair(0, 0, 1), partner))
    for line_step in range(1, chips):
        direct[line_step - 1].wait_recv()
        block = place(chip_at(-line_step), own_tp)
        for step in range(1, tp_count):
            planar[(line_step, step)] = send(
                block, block, *pair(line_step, step, 0), plane[step - 1]
            )
        copies.append(send(block, block, *pair(line_step, 0, 1), partner))
    for line_step in range(chips):
        for step in range(1, tp_count):
            planar[(line_step, step)].wait_recv()
            block = place(chip_at(-line_step), tp_at(-step))
            copies.append(send(block, block, *pair(line_step, step, 1), partner))
    own.wait()
    for copy in direct:
        copy.wait_send()
    for copy in planar.values():
        copy.wait_send()
    for copy in copies:
        copy.wait()


def spread(block, ident):
    count, tp_count = lax.axis_size("ep"), lax.axis_size("tp")
    rows, width = block.shape
    return pl.pallas_call(
        functools.partial(spread_body, count, tp_count),
        out_shape=jax.ShapeDtypeStruct((count, rows, width * tp_count), block.dtype),
        in_specs=[VMEM],
        out_specs=VMEM,
        scratch_shapes=[
            pltpu.SemaphoreType.DMA((2, count // 2, tp_count)),
            pltpu.SemaphoreType.DMA((2, count // 2, tp_count)),
            pltpu.SemaphoreType.DMA,
        ],
        compiler_params=pltpu.CompilerParams(collective_id=ident, has_side_effects=True),
    )(block)


def side_by_side(gathered):
    return jnp.concatenate([gathered[i] for i in range(gathered.shape[0])], -1)


def row_moments(values, ident):
    sums = jnp.stack([jnp.sum(values, -1), jnp.sum(values * values, -1)])
    (every,) = gather([sums], "tp", ident)
    totals = jnp.sum(every, 0)
    return totals[0][:, None], totals[1][:, None]


def on_device(
    tokens,
    retention_state,
    lengths,
    query_weight,
    key_weight,
    value_weight,
    gate_weight,
    out_weight,
    first_gain,
    routing,
    route_weight,
    expert_gate,
    expert_up,
    expert_down,
    shared_gate,
    shared_up,
    shared_down,
    side_gate,
    side_up,
    side_down,
    side_switch,
    second_gain,
):
    seq_rows = tokens.shape[0]
    model_width = tokens.shape[1]
    head_count = retention_state.shape[1]
    col_count = out_weight.shape[1]
    ep_count = lax.axis_size("ep")
    tp_rank = lax.axis_index("tp")
    ep_rank = lax.axis_index("ep")
    col_start = tp_rank * col_count
    side_width = side_gate.shape[1]
    side_part = jnp.concatenate([side_gate, side_up], 1)
    side_both, every_route, every_weight, *projections = first(
        [side_part, routing.T, route_weight.T],
        tokens,
        [query_weight, key_weight, value_weight, gate_weight],
        0,
    )
    side_both = side_both.reshape(model_width, 2 * side_width)
    mixed_heads, new_state = retain(
        retention_state, lengths, projections, tp_rank * head_count
    )
    (every_mixed,) = gather([mixed_heads], "tp", 1)
    mixing = jnp.dot(
        side_by_side(every_mixed),
        out_weight,
        preferred_element_type=jnp.float32,
    )
    own_cols = lax.dynamic_slice_in_dim(tokens, col_start, col_count, 1).astype(jnp.float32)
    pre_first = RESIDUAL_SCALE * own_cols + mixing
    first_sum, first_square = row_moments(pre_first, 2)
    row_mean = first_sum / model_width
    square = first_square / model_width
    own_gain = lax.dynamic_slice_in_dim(first_gain, col_start, col_count, 0)
    normed_cols = (
        (pre_first - row_mean) * lax.rsqrt(square - row_mean * row_mean + NORM_EPS) * own_gain
    ).astype(jnp.bfloat16)
    every_rows = spread(normed_cols, 3)
    normed_full = lax.dynamic_index_in_dim(every_rows, ep_rank, 0, keepdims=False)
    every_rows = every_rows.reshape(ep_count * seq_rows, model_width)

    local_experts = expert_gate.shape[0]
    top_count = routing.shape[1]
    expert_count = local_experts * ep_count
    capacity = (3 * seq_rows * top_count + expert_count - 1) // expert_count
    total_rows = ep_count * seq_rows
    route_all = jnp.transpose(every_route, (1, 0, 2)).reshape(top_count, total_rows)
    weight_all = jnp.transpose(every_weight, (1, 0, 2)).reshape(top_count, total_rows)
    local_ids = ep_rank * local_experts + jnp.arange(local_experts, dtype=jnp.int32)
    named = route_all[None, :, :] == local_ids[:, None, None]
    member = jnp.any(named, 1)
    pair_weight = jnp.sum(jnp.where(named, weight_all[None, :, :], 0.0), 1)
    index = jnp.arange(total_rows, dtype=jnp.int32)
    group = index // seq_rows
    earlier = ((index[:, None] < index[None, :]) & (group[:, None] == group[None, :])).astype(
        jnp.bfloat16
    )
    before = jnp.dot(
        member.astype(jnp.bfloat16), earlier, preferred_element_type=jnp.float32
    ).astype(jnp.int32)
    slot = jnp.where(member, group[None, :] * capacity + before, -1)
    slot_total = ep_count * capacity
    hit = slot[:, None, :] == jnp.arange(slot_total, dtype=jnp.int32)[None, :, None]
    table = hit.astype(jnp.bfloat16).reshape(local_experts * slot_total, total_rows)
    slot_weight = jnp.sum(jnp.where(hit, pair_weight[:, None, :], 0.0), -1, keepdims=True)
    chosen = (
        jnp.dot(table, every_rows, preferred_element_type=jnp.float32)
        .astype(jnp.bfloat16)
        .reshape(local_experts, slot_total, model_width)
    )
    gate_part = jnp.einsum("jcd,jdf->jcf", chosen, expert_gate, preferred_element_type=jnp.float32)
    up_part = jnp.einsum("jcd,jdf->jcf", chosen, expert_up, preferred_element_type=jnp.float32)
    hidden = (jax.nn.silu(gate_part) * up_part * slot_weight).astype(jnp.bfloat16)

    side_pre = jnp.dot(normed_full, side_both, preferred_element_type=jnp.float32)
    side_hidden = (jax.nn.silu(side_pre[:, :side_width]) * side_pre[:, side_width:]).astype(
        jnp.bfloat16
    )
    shared_hidden = (
        jax.nn.silu(jnp.dot(normed_full, shared_gate, preferred_element_type=jnp.float32))
        * jnp.dot(normed_full, shared_up, preferred_element_type=jnp.float32)
    ).astype(jnp.bfloat16)
    hidden_blocks, shared_blocks, side_blocks = gather(
        [hidden.reshape(local_experts * slot_total, -1), shared_hidden, side_hidden], "tp", 4
    )
    hidden_all = side_by_side(hidden_blocks).reshape(local_experts, slot_total, -1)
    result = (
        jnp.einsum("jcf,jfd->jcd", hidden_all, expert_down, preferred_element_type=jnp.float32)
        .astype(jnp.bfloat16)
        .reshape(local_experts * slot_total, col_count)
    )
    summed = (
        lax.dot_general(
            table, result, (((0,), (0,)), ((), ())), preferred_element_type=jnp.float32
        )
        .astype(jnp.bfloat16)
        .reshape(ep_count, seq_rows, col_count)
    )
    returned = scatter(summed, 5)
    routed = jnp.sum(returned.astype(jnp.float32), 0)
    shared_out = jnp.dot(
        side_by_side(shared_blocks), shared_down, preferred_element_type=jnp.float32
    )
    side_out = jnp.dot(side_by_side(side_blocks), side_down, preferred_element_type=jnp.float32)
    switch = jax.nn.sigmoid(
        jnp.sum(normed_full.astype(jnp.float32) * side_switch.astype(jnp.float32)[None, :], -1)
    )
    pre_second = (
        RESIDUAL_SCALE * normed_cols.astype(jnp.float32)
        + routed
        + shared_out
        + switch[:, None] * side_out
    )
    second_sum, second_square = row_moments(pre_second, 6)
    mean_second = second_sum / model_width
    square_second = second_square / model_width
    output = (
        (pre_second - mean_second)
        * lax.rsqrt(square_second - mean_second * mean_second + NORM_EPS)
        * second_gain
    ).astype(jnp.bfloat16)
    return (output, new_state)


def solution(mesh):
    return jax.shard_map(
        on_device,
        mesh=mesh,
        in_specs=(
            P("ep", None),
            P("ep", "tp", None, None),
            P("ep"),
            P(None, "tp"),
            P(None, "tp"),
            P(None, "tp"),
            P(None, "tp"),
            P(None, "tp"),
            P(),
            P("ep", None),
            P("ep", None),
            P("ep", None, "tp"),
            P("ep", None, "tp"),
            P("ep", None, "tp"),
            P(None, "tp"),
            P(None, "tp"),
            P(None, "tp"),
            P("ep", "tp"),
            P("ep", "tp"),
            P(None, "tp"),
            P(),
            P("tp"),
        ),
        out_specs=(P("ep", "tp"), P("ep", "tp", None, None)),
        check_vma=False,
    )
```
